32 devices in a mesh: sp: 8 (over z, x), tp: 4 (over y, core).
Axes of the slice: x: 2, y: 2, z: 4, core: 2. Of those that a mesh axis runs over, the one named last changes fastest.
Arguments:
- moe_input: bfloat16 [2048, 2048], P('sp'), may hold values from -6 to 6
- cotangent: bfloat16 [2048, 2048], P('sp'), may hold values from -6 to 6
- expert_ids: int32 [2048, 2], P('sp'), may hold values from 0 to 7, as said below
- route_weights: float32 [2048, 2], P('sp'), may hold values from 0.05 to 1
- gate_weight: bfloat16 [8, 2048, 1024], P('sp', None, 'tp'), may hold values from -0.125 to 0.125
- up_weight: bfloat16 [8, 2048, 1024], P('sp', None, 'tp'), may hold values from -0.125 to 0.125
- down_weight: bfloat16 [8, 1024, 2048], P('sp', 'tp'), may hold values from -0.1875 to 0.1875
- out_weight: bfloat16 [2048, 1024], P(None, 'tp'), may hold values from -0.1875 to 0.1875
- mixer_out: bfloat16 [2048, 1024], P('sp', 'tp'), may hold values from -6 to 6
- query_vectors: bfloat16 [2048, 512], P('sp', 'tp'), may hold values from -0.62109375 to 0.62109375
- key_vectors: bfloat16 [2048, 512], P('sp', 'tp'), may hold values from -0.62109375 to 0.62109375
- value_vectors: bfloat16 [2048, 1024], P('sp', 'tp'), may hold values from -6 to 6
- log_decay: float32 [2048, 512], P('sp', 'tp'), may hold values from -2 to 0
Outputs:
- grad_gate: bfloat16 [8, 2048, 1024], P('sp', None, 'tp')
- grad_up: bfloat16 [8, 2048, 1024], P('sp', None, 'tp')
- grad_down: bfloat16 [8, 1024, 2048], P('sp', 'tp')
- grad_out_weight: float32 [2048, 1024], P('sp', 'tp')
- grad_queries: bfloat16 [2048, 512], P('sp', 'tp')
- grad_keys: bfloat16 [2048, 512], P('sp', 'tp')
- grad_values: bfloat16 [2048, 1024], P('sp', 'tp')
- grad_log_decay: float32 [2048, 512], P('sp', 'tp')
The draws below stay inside these ranges and needn't reach their ends.
Inputs may be any that keep to these rules, and one draw needn't show every extreme that they name: `expert_ids`: each row names two different experts of one group, expert e lying in group e // 2. Each aligned block of 256 rows names every expert exactly 64 times and has equally many rows in each of the 4 groups.
All inputs are finite; a program needn't handle non-finite values.
Results may differ from the reference program's by a relative error of at most 0.01145.
Values may be sent and summed in bfloat16 or wider, within the bound.
A program may use at most 64 MiB of HBM per device.

```python
import math
import jax
import jax.numpy as jnp
from jax import lax

D = 2048
ATTENTION_HEADS = 8
KEY_CHANNELS = 64
VAL_DIM = 128
EXP_HIDDEN = 1024
GROUPS = 4
BLOCK = 64
TOK_DEV = 256
SEQUENCE_TOKENS = 2048
EXPERTS = 8
KEY_WIDTH = 512
VAL_WIDTH = 1024
N_TP = 4


def draw_expert_ids(key, part):
    block_total = SEQUENCE_TOKENS // TOK_DEV
    per_group = EXPERTS // GROUPS
    block_keys = jax.random.split(key, block_total)

    def one_block(block_key):
        keys_here = jax.random.split(block_key, 3)
        shuffled = jax.random.permutation(keys_here[0], TOK_DEV).astype(jnp.int32)
        group_of = shuffled % GROUPS
        rank_of = shuffled // GROUPS
        shifts = jax.random.randint(keys_here[1], (GROUPS,), 0, per_group)
        offsets = jax.random.randint(keys_here[2], (GROUPS,), 0, per_group - 1)
        first_pick = (rank_of + shifts[group_of]) % per_group
        second_pick = (first_pick + 1 + offsets[group_of]) % per_group
        return jnp.stack([group_of * per_group + first_pick, group_of * per_group + second_pick], axis=1)
    return jax.vmap(one_block)(block_keys).reshape(SEQUENCE_TOKENS, 2).astype(jnp.int32)


def draw_log_decay(key, part):
    channels = ATTENTION_HEADS * KEY_CHANNELS
    block_total = SEQUENCE_TOKENS // TOK_DEV
    key_sequence = jax.random.split(key, 7)
    fast_share = 0.5
    fast_mask = jax.random.uniform(key_sequence[0], (channels,)) < fast_share
    slow_rate = jnp.exp(jax.random.uniform(key_sequence[1], (channels,), minval=math.log(0.05), maxval=math.log(0.3))) / SEQUENCE_TOKENS
    fast_rate = jnp.exp(jax.random.uniform(key_sequence[2], (channels,), minval=math.log(0.01), maxval=math.log(1.0 / 30.0)))
    baseline_rate = jnp.where(fast_mask, fast_rate, slow_rate)
    hardware_factor = jnp.exp(jax.random.uniform(key_sequence[3], (block_total,), minval=math.log(0.5), maxval=math.log(2.0)))
    hardware_factor = jnp.repeat(hardware_factor, TOK_DEV)
    random_noise = 1.0 + 0.5 * jax.random.uniform(key_sequence[4], (SEQUENCE_TOKENS, channels), minval=-1.0, maxval=1.0)
    spike_locations = jax.random.randint(key_sequence[5], (2, ATTENTION_HEADS), 0, SEQUENCE_TOKENS)
    spike_size = jax.random.uniform(key_sequence[6], (2, ATTENTION_HEADS), minval=math.log(0.6), maxval=math.log(0.8))
    token_positions = jnp.arange(SEQUENCE_TOKENS, dtype=jnp.int32)
    spike_hits = (token_positions[:, None, None] == spike_locations[None, :, :]).astype(jnp.float32)
    spike_events = jnp.sum(spike_hits * spike_size[None, :, :], axis=1)
    spike_events = jnp.repeat(spike_events, KEY_CHANNELS, axis=1)
    return (spike_events - baseline_rate[None, :] * hardware_factor[:, None] * random_noise).astype(jnp.float32)


def spiked(array, key, source, target, shards_of, factor):
    owner, partner = [(jnp.arange(array.shape[position]) // (array.shape[position] // shards_of)).reshape([-1 if axis == position else 1 for axis in range(array.ndim)]) for position in (source, target)]
    chosen = jax.random.permutation(key, shards_of)[partner]
    strong = (owner == chosen) | (owner == (partner + shards_of // 2) % shards_of)
    return jnp.where(strong, factor * array, array)


def levels(own_key, shape, shards, least, high):
    def one(dim, shards_of):
        draws = jax.random.uniform(jax.random.fold_in(jax.random.fold_in(own_key, 6), dim), (shards_of,), jnp.float32, least / len(shards), high / len(shards))
        return jnp.repeat(jnp.exp(draws), shape[dim] // shards_of).reshape((-1,) + (1,) * (len(shape) - dim - 1))

    factor_of = one(*shards[0])
    for cut in shards[1:]:
        factor_of = factor_of * one(*cut)
    return factor_of


def bell_draw(rng, shape, scale, limit, shards=(), kind=jnp.bfloat16):
    factor_of = levels(rng, shape, shards, -0.22, 0.18) if shards else 1.0
    entries = jax.random.normal(rng, shape, jnp.float32) * scale * factor_of
    return jnp.minimum(jnp.maximum(entries, -limit), limit).astype(kind)


def gaussian_with(stream_key, extent, deviation, most, pieces, heavy, kind=jnp.bfloat16):
    entries = deviation * jax.random.normal(stream_key, extent, jnp.float32)
    if pieces:
        entries = entries * levels(stream_key, extent, pieces, -0.22, 0.18)
    return jnp.clip(spiked(entries, jax.random.fold_in(stream_key, 3), *heavy), -most, most).astype(kind)


def setup_inputs(seed: int = 0) -> dict:
    key_list = jax.random.split(jax.random.key(seed), 14)
    return {
        "moe_input": bell_draw(key_list[0], (SEQUENCE_TOKENS, D), 1.0, 6.0, ((0, 8),)),
        "cotangent": gaussian_with(key_list[1], (SEQUENCE_TOKENS, D), 1.0, 6.0, ((0, 8),), (0, 1, 8, 2.0)),
        "expert_ids": draw_expert_ids(jax.random.fold_in(key_list[13], 71), 0),
        "route_weights": jnp.clip(0.05 + 0.95 * jax.random.uniform(key_list[3], (SEQUENCE_TOKENS, 2), jnp.float32) ** levels(key_list[3], (SEQUENCE_TOKENS, 2), ((0, 8),), -0.2, 0.2), 0.05, 1.0),
        "gate_weight": bell_draw(key_list[4], (EXPERTS, D, EXP_HIDDEN), D ** -0.5, 0.125, ((0, 8), (2, 4))),
        "up_weight": bell_draw(key_list[5], (EXPERTS, D, EXP_HIDDEN), D ** -0.5, 0.125, ((0, 8), (2, 4))),
        "down_weight": bell_draw(key_list[6], (EXPERTS, EXP_HIDDEN, D), EXP_HIDDEN ** -0.5, 0.1875, ((0, 8), (1, 4))),
        "out_weight": bell_draw(key_list[7], (D, VAL_WIDTH), VAL_WIDTH ** -0.5, 0.1875, ((1, 4),)),
        "mixer_out": bell_draw(key_list[8], (SEQUENCE_TOKENS, VAL_WIDTH), 1.0, 6.0, ((0, 8), (1, 4))),
        "query_vectors": bell_draw(key_list[9], (SEQUENCE_TOKENS, KEY_WIDTH), (0.7 * SEQUENCE_TOKENS ** -0.25), 0.62109375, ((0, 8), (1, 4))),
        "key_vectors": bell_draw(key_list[10], (SEQUENCE_TOKENS, KEY_WIDTH), (0.7 * SEQUENCE_TOKENS ** -0.25), 0.62109375, ((0, 8), (1, 4))),
        "value_vectors": bell_draw(key_list[11], (SEQUENCE_TOKENS, VAL_WIDTH), 1.0, 6.0, ((0, 8), (1, 4))),
        "log_decay": draw_log_decay(jax.random.fold_in(key_list[13], 71), 0),
    }


HIGHEST = lax.Precision.HIGHEST

def block_step(memory, inputs):
    query_block, key_block, value_block, decay_block = inputs
    block_len = query_block.shape[1]
    causal = jnp.tril(jnp.ones((block_len, block_len), dtype=bool))
    cumulative = jnp.cumsum(decay_block, axis=1)
    carried = jnp.einsum('hcd,hdv->hcv', query_block * jnp.exp(cumulative), memory, precision=HIGHEST)
    difference = cumulative[:, :, None, :] - cumulative[:, None, :, :]
    decay = jnp.exp(jnp.where(causal[None, :, :, None], difference, -jnp.inf))
    scores = jnp.einsum('htd,hsd,htsd->hts', query_block, key_block, decay, precision=HIGHEST)
    within = jnp.einsum('hts,hsv->htv', scores, value_block, precision=HIGHEST)
    final_row = cumulative[:, -1:, :]
    memory = jnp.exp(final_row[:, 0, :])[:, :, None] * memory + jnp.einsum('hsd,hsv->hdv', key_block * jnp.exp(final_row - cumulative), value_block, precision=HIGHEST)
    return (memory, carried + within)

def run_blocks(query_heads, key_heads, value_heads, decay_heads, memory):
    head_count = query_heads.shape[0]
    length = query_heads.shape[1]
    block_count = length // BLOCK

    def to_blocks(matrix):
        return matrix.reshape(head_count, block_count, BLOCK, matrix.shape[-1]).transpose(1, 0, 2, 3)
    memory, outputs = lax.scan(jax.checkpoint(block_step), memory, (to_blocks(query_heads), to_blocks(key_heads), to_blocks(value_heads), to_blocks(decay_heads)))
    return (outputs.transpose(1, 0, 2, 3).reshape(head_count, length, outputs.shape[-1]), memory)

def expert_backward(inputs):
    routed, routed_cot, gate_local, up_local, down_local = inputs
    pre_gate = jnp.dot(routed, gate_local, preferred_element_type=jnp.float32)
    pre_up = jnp.dot(routed, up_local, preferred_element_type=jnp.float32)
    sigmoid_gate = jax.nn.sigmoid(pre_gate)
    activated = pre_gate * sigmoid_gate
    hidden = (activated * pre_up).astype(jnp.bfloat16)
    delta_hidden = jnp.dot(routed_cot, down_local.T, preferred_element_type=jnp.float32)
    grad_down = jnp.dot(hidden.T, routed_cot, preferred_element_type=jnp.float32).astype(jnp.bfloat16)
    delta_gate = (delta_hidden * pre_up * sigmoid_gate * (1.0 + pre_gate * (1.0 - sigmoid_gate))).astype(jnp.bfloat16)
    delta_up = (delta_hidden * activated).astype(jnp.bfloat16)
    grad_gate = jnp.dot(routed.T, delta_gate, preferred_element_type=jnp.float32).astype(jnp.bfloat16)
    grad_up = jnp.dot(routed.T, delta_up, preferred_element_type=jnp.float32).astype(jnp.bfloat16)
    unit_span = gate_local.shape[1] // N_TP
    summed = jnp.zeros((routed.shape[0], routed.shape[1]), jnp.float32)
    for member in range(N_TP):
        lower_unit = member * unit_span
        upper_unit = lower_unit + unit_span
        partial_value = jnp.dot(delta_gate[:, lower_unit:upper_unit], gate_local[:, lower_unit:upper_unit].T, preferred_element_type=jnp.float32)
        partial_value = partial_value + jnp.dot(delta_up[:, lower_unit:upper_unit], up_local[:, lower_unit:upper_unit].T, preferred_element_type=jnp.float32)
        summed = summed + lax.optimization_barrier(partial_value.astype(jnp.bfloat16)).astype(jnp.float32)
    return (grad_gate, grad_up, grad_down, summed.astype(jnp.bfloat16))

def reference(moe_input, cotangent, expert_ids, route_weights, gate_weight, up_weight, down_weight, out_weight, mixer_out, query_vectors, key_vectors, value_vectors, log_decay):
    tok_count = moe_input.shape[0]
    model_width = moe_input.shape[1]
    expert_count = gate_weight.shape[0]
    slot_count = 2 * tok_count // expert_count
    flat_ids = expert_ids.reshape(-1).astype(jnp.int32)
    sorting = jnp.argsort(flat_ids, stable=True).astype(jnp.int32)
    source_rows = (sorting // 2).astype(jnp.int32)
    scaled = (route_weights[:, :, None] * cotangent[:, None, :].astype(jnp.float32)).astype(jnp.bfloat16)
    scaled = scaled.reshape(2 * tok_count, model_width)
    rows_in = moe_input[source_rows].reshape(expert_count, slot_count, model_width)
    rows_cot = scaled[sorting].reshape(expert_count, slot_count, model_width)
    grad_gate, grad_up, grad_down, returned = lax.map(expert_backward, (rows_in, rows_cot, gate_weight, up_weight, down_weight))
    inverse = jnp.argsort(sorting).astype(jnp.int32)
    per_slot = returned.reshape(2 * tok_count, model_width)[inverse].reshape(tok_count, 2, model_width)
    per_slot = per_slot.astype(jnp.float32)
    token_grad = (cotangent.astype(jnp.float32) + per_slot[:, 0] + per_slot[:, 1]).astype(jnp.bfloat16)
    mixer_grad = jnp.dot(token_grad, out_weight, preferred_element_type=jnp.float32).astype(jnp.bfloat16)
    grad_out_weight = jnp.dot(token_grad.T, mixer_out, preferred_element_type=jnp.float32)

    def heads_first(matrix, channel_size):
        return matrix.astype(jnp.float32).reshape(tok_count, ATTENTION_HEADS, channel_size).transpose(1, 0, 2)

    def tokens_first(matrix):
        return matrix.transpose(1, 0, 2).reshape(tok_count, -1)

    def forward(query_in, key_in, value_in, decay_in):
        initial = jnp.zeros((ATTENTION_HEADS, KEY_CHANNELS, VAL_DIM), jnp.float32)
        return run_blocks(query_in * KEY_CHANNELS ** (-0.5), key_in, value_in, decay_in, initial)[0]
    pullback = jax.vjp(forward, heads_first(query_vectors, KEY_CHANNELS), heads_first(key_vectors, KEY_CHANNELS), heads_first(value_vectors, VAL_DIM), heads_first(log_decay, KEY_CHANNELS))[1]
    grads = pullback(heads_first(mixer_grad, VAL_DIM))
    return (grad_gate, grad_up, grad_down, grad_out_weight, tokens_first(grads[0]).astype(jnp.bfloat16), tokens_first(grads[1]).astype(jnp.bfloat16), tokens_first(grads[2]).astype(jnp.bfloat16), tokens_first(grads[3]).astype(jnp.float32))
```

```python
import functools
import jax
import jax.numpy as jnp
from jax import lax
from jax.experimental import pallas as pl
from jax.experimental.pallas import tpu as pltpu
from jax.sharding import PartitionSpec as P

KEY_CHANNELS = 64
VAL_DIM = 128
BLOCK = 64
HIGHEST = lax.Precision.HIGHEST
F32 = jnp.float32
BF16 = jnp.bfloat16


def mm(a, b, ca=1, cb=0, precision=None):
    return lax.dot_general(
        a, b, (((ca,), (cb,)), ((), ())), precision=precision, preferred_element_type=F32
    )


def expert_pass(routed, routed_cot, gate_local, up_local, down_local):
    pre_gate = jnp.dot(routed, gate_local, preferred_element_type=jnp.float32)
    pre_up = jnp.dot(routed, up_local, preferred_element_type=jnp.float32)
    sigmoid_gate = jax.nn.sigmoid(pre_gate)
    activated = pre_gate * sigmoid_gate
    hidden = (activated * pre_up).astype(jnp.bfloat16)
    delta_hidden = jnp.dot(routed_cot, down_local.T, preferred_element_type=jnp.float32)
    grad_down = jnp.dot(hidden.T, routed_cot, preferred_element_type=jnp.float32).astype(
        jnp.bfloat16
    )
    delta_gate = (
        delta_hidden * pre_up * sigmoid_gate * (1.0 + pre_gate * (1.0 - sigmoid_gate))
    ).astype(jnp.bfloat16)
    delta_up = (delta_hidden * activated).astype(jnp.bfloat16)
    grad_gate = jnp.dot(routed.T, delta_gate, preferred_element_type=jnp.float32).astype(
        jnp.bfloat16
    )
    grad_up = jnp.dot(routed.T, delta_up, preferred_element_type=jnp.float32).astype(jnp.bfloat16)
    partial_value = jnp.dot(delta_gate, gate_local.T, preferred_element_type=jnp.float32)
    partial_value = partial_value + jnp.dot(
        delta_up, up_local.T, preferred_element_type=jnp.float32
    )
    return (grad_gate, grad_up, grad_down, partial_value)


def greet(n, axis):
    me = lax.axis_index(axis)
    barrier = pltpu.get_barrier_semaphore()

    def body(d, _):
        pl.semaphore_signal(barrier, inc=1, device_id={axis: lax.rem(me + d, n)})
        return 0

    lax.fori_loop(1, n, body, 0)
    return barrier


def attention_kernel(
    n, tg, ow, mo, q, k, v, a, gq, gk, gv, ga, gow,
    pay, recv, gsend, grecv, upd_s, upd_p, ssem, rsem, gssem, grsem,
):
    me = lax.axis_index("sp")
    barrier = greet(n, "sp")
    tokens, lanes = q.shape
    blocks = tokens // BLOCK
    width = v.shape[1]
    heads = width // VAL_DIM
    rows = gow.shape[0]
    scale = KEY_CHANNELS ** (-0.5)

    cot = mm(tg[...], ow[...]).astype(BF16)
    row = lax.broadcasted_iota(jnp.int32, (tokens, tokens), 0)
    col = lax.broadcasted_iota(jnp.int32, (tokens, tokens), 1)
    same = (row // BLOCK) == (col // BLOCK)
    causal = same & (col <= row)
    cum = mm(jnp.where(causal, 1.0, 0.0), a[...], precision=HIGHEST)

    def spread(at):
        return jnp.concatenate(
            [
                jnp.broadcast_to(cum[b * BLOCK + at : b * BLOCK + at + 1], (BLOCK, lanes))
                for b in range(blocks)
            ],
            axis=0,
        )

    mid = spread(BLOCK // 2 - 1)
    end = spread(BLOCK - 1)
    qf = q[...].astype(F32) * scale
    kf = k[...].astype(F32)
    up_mid = jnp.exp(cum - mid)
    down_mid = jnp.exp(mid - cum)
    from_start = jnp.exp(cum)
    to_end = jnp.exp(end - cum)
    q_mid = (qf * up_mid).astype(BF16)
    k_mid = (kf * down_mid).astype(BF16)
    q_start = (qf * from_start).astype(BF16)
    k_end = (kf * to_end).astype(BF16)
    total = [cum[(b + 1) * BLOCK - 1 : (b + 1) * BLOCK] for b in range(blocks)]
    keep = [jnp.exp(t) for t in total]
    hrow = lax.broadcasted_iota(jnp.int32, (width, lanes), 0) // VAL_DIM
    hcol = lax.broadcasted_iota(jnp.int32, (width, lanes), 1) // KEY_CHANNELS
    headed = hrow == hcol

    def part(x, b):
        return x[b * BLOCK : (b + 1) * BLOCK]

    values = v[...]
    for b in range(blocks):
        upd_s[b] = jnp.where(headed, mm(part(values, b), part(k_end, b), 0, 0), 0.0)
        upd_p[b] = jnp.where(headed, mm(part(cot, b), part(q_start, b), 0, 0), 0.0)
    state = jnp.zeros((width, lanes), F32)
    pull = jnp.zeros((width, lanes), F32)
    for b in range(blocks):
        state = keep[b] * state + upd_s[b]
    for b in reversed(range(blocks)):
        pull = keep[b] * pull + upd_p[b]
    kept = jnp.exp(functools.reduce(lambda x, y: x + y, total))
    kept_hi = kept.astype(BF16)
    kept_lo = (kept - kept_hi.astype(F32)).astype(BF16)
    tail = jnp.concatenate(
        [jnp.broadcast_to(kept_hi.astype(F32), (8, lanes)), jnp.broadcast_to(kept_lo.astype(F32), (8, lanes))],
        axis=0,
    ).astype(BF16)

    def compact(x):
        return functools.reduce(
            lambda s, t: s + t, [x[h * VAL_DIM : (h + 1) * VAL_DIM] for h in range(heads)]
        )

    def expand(x):
        return jnp.where(headed, jnp.concatenate([x] * heads, axis=0), 0.0)

    pay[0, :VAL_DIM, :] = compact(state).astype(BF16)
    pay[1, :VAL_DIM, :] = compact(pull).astype(BF16)
    pay[0, VAL_DIM:, :] = tail
    pay[1, VAL_DIM:, :] = tail
    for j in range(tg.shape[1] // 256):
        gsend[j * 256 : (j + 1) * 256, :] = mm(
            tg[:, j * 256 : (j + 1) * 256], mo[...], 0, 0
        ).astype(BF16)
    pl.semaphore_wait(barrier, n - 1)

    def state_copy(d, slot):
        p = lax.rem(me + d, n)
        return pltpu.make_async_remote_copy(
            src_ref=pay.at[jnp.where(p > me, 0, 1)],
            dst_ref=recv.at[slot],
            send_sem=ssem.at[d],
            recv_sem=rsem.at[slot],
            device_id={"sp": p},
        )

    def grad_copy(d, slot):
        p = lax.rem(me + d, n)
        return pltpu.make_async_remote_copy(
            src_ref=gsend.at[pl.ds(pl.multiple_of(p * rows, rows), rows)],
            dst_ref=grecv.at[slot],
            send_sem=gssem.at[d],
            recv_sem=grsem.at[slot],
            device_id={"sp": p},
        )

    def each(f):
        def body(d, _):
            f(d)
            return 0

        lax.fori_loop(1, n, body, 0)

    each(lambda d: state_copy(d, me).start())
    each(lambda d: grad_copy(d, me).start())

    head_lane = lax.broadcasted_iota(jnp.int32, (tokens, lanes), 1) // KEY_CHANNELS
    dq = jnp.zeros((tokens, lanes), F32)
    dk = jnp.zeros((tokens, lanes), F32)
    dv = []
    for h in range(heads):
        cot_h = cot[:, h * VAL_DIM : (h + 1) * VAL_DIM]
        val_h = values[:, h * VAL_DIM : (h + 1) * VAL_DIM]
        q_h = jnp.where(head_lane == h, qf * up_mid, 0.0).astype(BF16)
        scores = jnp.where(causal, mm(q_h, k_mid, 1, 1), 0.0).astype(BF16)
        dscores = jnp.where(causal, mm(cot_h, val_h, 1, 1), 0.0).astype(BF16)
        dq = jnp.where(head_lane == h, mm(dscores, k_mid), dq)
        dk = jnp.where(head_lane == h, mm(dscores, q_mid, 0, 0), dk)
        dv.append(mm(scores, cot_h, 0, 0))
    dq = dq * up_mid
    dk = dk * down_mid
    dv = jnp.concatenate(dv, axis=1)

    each(lambda d: state_copy(d, lax.rem(me + d, n)).wait_recv())

    def follow(p, carry):
        ends = recv[p, VAL_DIM:, :].astype(F32)
        return (ends[0:1] + ends[8:9]) * carry + recv[p, :VAL_DIM, :].astype(F32)

    zero = jnp.zeros((VAL_DIM, lanes), F32)
    state = expand(lax.fori_loop(0, me, follow, zero))
    pull = expand(lax.fori_loop(0, n - 1 - me, lambda i, c: follow(n - 1 - i, c), zero))
    dq_in, after = [], []
    for b in range(blocks):
        dq_in.append(mm(part(cot, b), state.astype(BF16)))
        state = keep[b] * state + upd_s[b]
        after.append(state)
    dk_in, dv_in, edge = [None] * blocks, [None] * blocks, [None] * blocks
    for b in reversed(range(blocks)):
        low = pull.astype(BF16)
        dk_in[b] = mm(part(values, b), low)
        dv_in[b] = mm(part(k_end, b), low, 1, 1)
        edge[b] = jnp.broadcast_to(
            jnp.sum(after[b] * pull, axis=0, keepdims=True), (BLOCK, lanes)
        )
        pull = keep[b] * pull + upd_p[b]
    dq = dq + jnp.concatenate(dq_in, axis=0) * from_start
    dk = dk + jnp.concatenate(dk_in, axis=0) * to_end
    dv = dv + jnp.concatenate(dv_in, axis=0)
    gq[...] = (dq * scale).astype(BF16)
    gk[...] = dk.astype(BF16)
    gv[...] = dv.astype(BF16)
    flux = qf * dq - kf * dk
    later = jnp.where(same & (col >= row), 1.0, 0.0)
    ga[...] = mm(later, flux, precision=HIGHEST) + jnp.concatenate(edge, axis=0)

    each(lambda d: grad_copy(d, lax.rem(me + d, n)).wait_recv())
    own = gsend[pl.ds(pl.multiple_of(me * rows, rows), rows), :].astype(F32)
    gow[...] = lax.fori_loop(
        1, n, lambda d, t: t + grecv[lax.rem(me + d, n)].astype(F32), own
    )
    each(lambda d: state_copy(d, me).wait_send())
    each(lambda d: grad_copy(d, me).wait_send())


def attention_backward(token_grad, out_weight, mixer_out, query, key, value, log_decay):
    n = lax.axis_size("sp")
    tokens, lanes = query.shape
    width = value.shape[1]
    model = token_grad.shape[1]
    rows = model // n
    vm = pl.BlockSpec(memory_space=pltpu.VMEM)
    return pl.pallas_call(
        functools.partial(attention_kernel, n),
        out_shape=(
            jax.ShapeDtypeStruct((tokens, lanes), BF16),
            jax.ShapeDtypeStruct((tokens, lanes), BF16),
            jax.ShapeDtypeStruct((tokens, width), BF16),
            jax.ShapeDtypeStruct((tokens, lanes), F32),
            jax.ShapeDtypeStruct((rows, mixer_out.shape[1]), F32),
        ),
        in_specs=[vm] * 7,
        out_specs=(vm,) * 5,
        scratch_shapes=[
            pltpu.VMEM((2, VAL_DIM + 16, lanes), BF16),
            pltpu.VMEM((n, VAL_DIM + 16, lanes), BF16),
            pltpu.VMEM((model, mixer_out.shape[1]), BF16),
            pltpu.VMEM((n, rows, mixer_out.shape[1]), BF16),
            pltpu.VMEM((tokens // BLOCK, width, lanes), F32),
            pltpu.VMEM((tokens // BLOCK, width, lanes), F32),
            pltpu.SemaphoreType.DMA((n,)),
            pltpu.SemaphoreType.DMA((n,)),
            pltpu.SemaphoreType.DMA((n,)),
            pltpu.SemaphoreType.DMA((n,)),
        ],
        compiler_params=pltpu.CompilerParams(
            collective_id=0, has_side_effects=True, vmem_limit_bytes=24 * 1024 * 1024
        ),
        cost_estimate=pl.CostEstimate(
            flops=2 * 10**9, bytes_accessed=4 * 10**6, transcendentals=10**5
        ),
    )(token_grad, out_weight, mixer_out, query, key, value, log_decay)


def shards(
    moe_input,
    cotangent,
    expert_ids,
    route_weights,
    gate_weight,
    up_weight,
    down_weight,
    out_weight,
    mixer_out,
    query_vectors,
    key_vectors,
    value_vectors,
    log_decay,
):
    tok_count = moe_input.shape[0]
    model_width = moe_input.shape[1]
    slot_total = 2 * tok_count
    flat_ids = expert_ids.reshape(-1)
    sorting = jnp.argsort(flat_ids, stable=True)
    source_rows = sorting // 2
    inverse = jnp.argsort(sorting)
    gate_local = gate_weight[0]
    up_local = up_weight[0]
    down_local = down_weight[0]
    quarter = model_width // lax.axis_size("tp")
    offset = lax.axis_index("tp") * quarter
    own_input = lax.dynamic_slice_in_dim(moe_input, offset, quarter, 1)
    own_cot = lax.dynamic_slice_in_dim(cotangent, offset, quarter, 1)
    own_scaled = (route_weights[:, :, None] * own_cot[:, None, :].astype(jnp.float32)).astype(
        jnp.bfloat16
    )
    own_scaled = own_scaled.reshape(slot_total, quarter)
    arrived = (
        lax.all_to_all(own_input[source_rows], "sp", split_axis=0, concat_axis=0, tiled=True),
        lax.all_to_all(own_scaled[sorting], "sp", split_axis=0, concat_axis=0, tiled=True),
    )
    routed, routed_cot = (
        lax.all_gather(arrived[0], "tp", axis=1, tiled=True),
        lax.all_gather(arrived[1], "tp", axis=1, tiled=True),
    )
    grad_gate, grad_up, grad_down, partial_value = expert_pass(
        routed, routed_cot, gate_local, up_local, down_local
    )
    summed = lax.psum_scatter(
        partial_value.astype(jnp.bfloat16), "tp", scatter_dimension=1, tiled=True
    )
    returned = lax.all_to_all(summed, "sp", split_axis=0, concat_axis=0, tiled=True)
    per_slot = returned[inverse].reshape(tok_count, 2, quarter).astype(jnp.float32)
    own_grad = (own_cot.astype(jnp.float32) + per_slot[:, 0] + per_slot[:, 1]).astype(jnp.bfloat16)
    token_grad = lax.all_gather(own_grad, "tp", axis=1, tiled=True)
    gradients = attention_backward(
        token_grad, out_weight, mixer_out, query_vectors, key_vectors, value_vectors, log_decay
    )
    return (
        grad_gate[None],
        grad_up[None],
        grad_down[None],
        gradients[4],
        gradients[0],
        gradients[1],
        gradients[2],
        gradients[3],
    )


def solution(mesh):
    return jax.shard_map(
        shards,
        mesh=mesh,
        in_specs=(
            P("sp", None),
            P("sp", None),
            P("sp", None),
            P("sp", None),
            P("sp", None, "tp"),
            P("sp", None, "tp"),
            P("sp", "tp", None),
            P(None, "tp"),
            P("sp", "tp"),
            P("sp", "tp"),
            P("sp", "tp"),
            P("sp", "tp"),
            P("sp", "tp"),
        ),
        out_specs=(
            P("sp", None, "tp"),
            P("sp", None, "tp"),
            P("sp", "tp", None),
            P("sp", "tp"),
            P("sp", "tp"),
            P("sp", "tp"),
            P("sp", "tp"),
            P("sp", "tp"),
        ),
        check_vma=False,
    )
```

```python
import functools
import jax
import jax.numpy as jnp
from jax import lax
from jax.experimental import pallas as pl
from jax.experimental.pallas import tpu as pltpu
from jax.sharding import PartitionSpec as P

KEY_CHANNELS = 64
VAL_DIM = 128
BLOCK = 64
HIGHEST = lax.Precision.HIGHEST
F32 = jnp.float32
BF16 = jnp.bfloat16


def mm(a, b, ca=1, cb=0, precision=None):
    return lax.dot_general(
        a, b, (((ca,), (cb,)), ((), ())), precision=precision, preferred_element_type=F32
    )


def expert_pass(routed, routed_cot, gate_local, up_local, down_local):
    pre_gate = jnp.dot(routed, gate_local, preferred_element_type=jnp.float32)
    pre_up = jnp.dot(routed, up_local, preferred_element_type=jnp.float32)
    sigmoid_gate = jax.nn.sigmoid(pre_gate)
    activated = pre_gate * sigmoid_gate
    hidden = (activated * pre_up).astype(jnp.bfloat16)
    delta_hidden = jnp.dot(routed_cot, down_local.T, preferred_element_type=jnp.float32)
    grad_down = jnp.dot(hidden.T, routed_cot, preferred_element_type=jnp.float32).astype(
        jnp.bfloat16
    )
    delta_gate = (
        delta_hidden * pre_up * sigmoid_gate * (1.0 + pre_gate * (1.0 - sigmoid_gate))
    ).astype(jnp.bfloat16)
    delta_up = (delta_hidden * activated).astype(jnp.bfloat16)
    grad_gate = jnp.dot(routed.T, delta_gate, preferred_element_type=jnp.float32).astype(
        jnp.bfloat16
    )
    grad_up = jnp.dot(routed.T, delta_up, preferred_element_type=jnp.float32).astype(jnp.bfloat16)
    partial_value = jnp.dot(delta_gate, gate_local.T, preferred_element_type=jnp.float32)
    partial_value = partial_value + jnp.dot(
        delta_up, up_local.T, preferred_element_type=jnp.float32
    )
    return (grad_gate, grad_up, grad_down, partial_value)


def greet(n, axis):
    me = lax.axis_index(axis)
    barrier = pltpu.get_barrier_semaphore()

    def body(d, _):
        pl.semaphore_signal(barrier, inc=1, device_id={axis: lax.rem(me + d, n)})
        return 0

    lax.fori_loop(1, n, body, 0)
    return barrier


def attention_kernel(
    n, tg, ow, mo, q, k, v, a, gq, gk, gv, ga, gow,
    pay, recv, gsend, grecv, upd_s, upd_p, ssem, rsem, gssem, grsem,
):
    me = lax.axis_index("sp")
    barrier = greet(n, "sp")
    tokens, lanes = q.shape
    blocks = tokens // BLOCK
    width = v.shape[1]
    heads = width // VAL_DIM
    rows = gow.shape[0]
    scale = KEY_CHANNELS ** (-0.5)

    cot = mm(tg[...], ow[...]).astype(BF16)
    row = lax.broadcasted_iota(jnp.int32, (tokens, tokens), 0)
    col = lax.broadcasted_iota(jnp.int32, (tokens, tokens), 1)
    same = (row // BLOCK) == (col // BLOCK)
    causal = same & (col <= row)
    cum = mm(jnp.where(causal, 1.0, 0.0), a[...], precision=HIGHEST)

    def spread(at):
        return jnp.concatenate(
            [
                jnp.broadcast_to(cum[b * BLOCK + at : b * BLOCK + at + 1], (BLOCK, lanes))
                for b in range(blocks)
            ],
            axis=0,
        )

    mid = spread(BLOCK // 2 - 1)
    end = spread(BLOCK - 1)
    qf = q[...].astype(F32) * scale
    kf = k[...].astype(F32)
    up_mid = jnp.exp(cum - mid)
    down_mid = jnp.exp(mid - cum)
    from_start = jnp.exp(cum)
    to_end = jnp.exp(end - cum)
    q_mid = (qf * up_mid).astype(BF16)
    k_mid = (kf * down_mid).astype(BF16)
    q_start = (qf * from_start).astype(BF16)
    k_end = (kf * to_end).astype(BF16)
    total = [cum[(b + 1) * BLOCK - 1 : (b + 1) * BLOCK] for b in range(blocks)]
    keep = [jnp.exp(t) for t in total]
    hrow = lax.broadcasted_iota(jnp.int32, (width, lanes), 0) // VAL_DIM
    hcol = lax.broadcasted_iota(jnp.int32, (width, lanes), 1) // KEY_CHANNELS
    headed = hrow == hcol

    def part(x, b):
        return x[b * BLOCK : (b + 1) * BLOCK]

    values = v[...]
    for b in range(blocks):
        upd_s[b] = jnp.where(headed, mm(part(values, b), part(k_end, b), 0, 0), 0.0)
        upd_p[b] = jnp.where(headed, mm(part(cot, b), part(q_start, b), 0, 0), 0.0)
    state = jnp.zeros((width, lanes), F32)
    pull = jnp.zeros((width, lanes), F32)
    for b in range(blocks):
        state = keep[b] * state + upd_s[b]
    for b in reversed(range(blocks)):
        pull = keep[b] * pull + upd_p[b]
    kept = jnp.exp(functools.reduce(lambda x, y: x + y, total))
    kept_hi = kept.astype(BF16)
    kept_lo = (kept - kept_hi.astype(F32)).astype(BF16)
    tail = jnp.concatenate(
        [jnp.broadcast_to(kept_hi.astype(F32), (8, lanes)), jnp.broadcast_to(kept_lo.astype(F32), (8, lanes))],
        axis=0,
    ).astype(BF16)

    def compact(x):
        return functools.reduce(
            lambda s, t: s + t, [x[h * VAL_DIM : (h + 1) * VAL_DIM] for h in range(heads)]
        )

    def expand(x):
        return jnp.where(headed, jnp.concatenate([x] * heads, axis=0), 0.0)

    pay[0, :VAL_DIM, :] = compact(state).astype(BF16)
    pay[1, :VAL_DIM, :] = compact(pull).astype(BF16)
    pay[0, VAL_DIM:, :] = tail
    pay[1, VAL_DIM:, :] = tail
    for j in range(tg.shape[1] // 256):
        gsend[j * 256 : (j + 1) * 256, :] = mm(
            tg[:, j * 256 : (j + 1) * 256], mo[...], 0, 0
        ).astype(BF16)
    pl.semaphore_wait(barrier, n - 1)

    def state_copy(d, slot):
        p = lax.rem(me + d, n)
        return pltpu.make_async_remote_copy(
            src_ref=pay.at[jnp.where(p > me, 0, 1)],
            dst_ref=recv.at[slot],
            send_sem=ssem.at[d],
            recv_sem=rsem.at[slot],
            device_id={"sp": p},
        )

    def grad_copy(d, slot):
        p = lax.rem(me + d, n)
        return pltpu.make_async_remote_copy(
            src_ref=gsend.at[pl.ds(pl.multiple_of(p * rows, rows), rows)],
            dst_ref=grecv.at[slot],
            send_sem=gssem.at[d],
            recv_sem=grsem.at[slot],
            device_id={"sp": p},
        )

    def each(f):
        def body(d, _):
            f(d)
            return 0

        lax.fori_loop(1, n, body, 0)

    each(lambda d: state_copy(d, me).start())
    each(lambda d: grad_copy(d, me).start())

    head_lane = lax.broadcasted_iota(jnp.int32, (tokens, lanes), 1) // KEY_CHANNELS
    dq = jnp.zeros((tokens, lanes), F32)
    dk = jnp.zeros((tokens, lanes), F32)
    dv = []
    for h in range(heads):
        cot_h = cot[:, h * VAL_DIM : (h + 1) * VAL_DIM]
        val_h = values[:, h * VAL_DIM : (h + 1) * VAL_DIM]
        q_h = jnp.where(head_lane == h, qf * up_mid, 0.0).astype(BF16)
        scores = jnp.where(causal, mm(q_h, k_mid, 1, 1), 0.0).astype(BF16)
        dscores = jnp.where(causal, mm(cot_h, val_h, 1, 1), 0.0).astype(BF16)
        dq = jnp.where(head_lane == h, mm(dscores, k_mid), dq)
        dk = jnp.where(head_lane == h, mm(dscores, q_mid, 0, 0), dk)
        dv.append(mm(scores, cot_h, 0, 0))
    dq = dq * up_mid
    dk = dk * down_mid
    dv = jnp.concatenate(dv, axis=1)

    each(lambda d: state_copy(d, lax.rem(me + d, n)).wait_recv())

    def follow(p, carry):
        ends = recv[p, VAL_DIM:, :].astype(F32)
        return (ends[0:1] + ends[8:9]) * carry + recv[p, :VAL_DIM, :].astype(F32)

    zero = jnp.zeros((VAL_DIM, lanes), F32)
    state = expand(lax.fori_loop(0, me, follow, zero))
    pull = expand(lax.fori_loop(0, n - 1 - me, lambda i, c: follow(n - 1 - i, c), zero))
    dq_in, after = [], []
    for b in range(blocks):
        dq_in.append(mm(part(cot, b), state.astype(BF16)))
        state = keep[b] * state + upd_s[b]
        after.append(state)
    dk_in, dv_in, edge = [None] * blocks, [None] * blocks, [None] * blocks
    for b in reversed(range(blocks)):
        low = pull.astype(BF16)
        dk_in[b] = mm(part(values, b), low)
        dv_in[b] = mm(part(k_end, b), low, 1, 1)
        edge[b] = jnp.broadcast_to(
            jnp.sum(after[b] * pull, axis=0, keepdims=True), (BLOCK, lanes)
        )
        pull = keep[b] * pull + upd_p[b]
    dq = dq + jnp.concatenate(dq_in, axis=0) * from_start
    dk = dk + jnp.concatenate(dk_in, axis=0) * to_end
    dv = dv + jnp.concatenate(dv_in, axis=0)
    gq[...] = (dq * scale).astype(BF16)
    gk[...] = dk.astype(BF16)
    gv[...] = dv.astype(BF16)
    flux = qf * dq - kf * dk
    later = jnp.where(same & (col >= row), 1.0, 0.0)
    ga[...] = mm(later, flux, precision=HIGHEST) + jnp.concatenate(edge, axis=0)

    each(lambda d: grad_copy(d, lax.rem(me + d, n)).wait_recv())
    own = gsend[pl.ds(pl.multiple_of(me * rows, rows), rows), :].astype(F32)
    gow[...] = lax.fori_loop(
        1, n, lambda d, t: t + grecv[lax.rem(me + d, n)].astype(F32), own
    )
    each(lambda d: state_copy(d, me).wait_send())
    each(lambda d: grad_copy(d, me).wait_send())


def attention_backward(token_grad, out_weight, mixer_out, query, key, value, log_decay):
    n = lax.axis_size("sp")
    tokens, lanes = query.shape
    width = value.shape[1]
    model = token_grad.shape[1]
    rows = model // n
    vm = pl.BlockSpec(memory_space=pltpu.VMEM)
    return pl.pallas_call(
        functools.partial(attention_kernel, n),
        out_shape=(
            jax.ShapeDtypeStruct((tokens, lanes), BF16),
            jax.ShapeDtypeStruct((tokens, lanes), BF16),
            jax.ShapeDtypeStruct((tokens, width), BF16),
            jax.ShapeDtypeStruct((tokens, lanes), F32),
            jax.ShapeDtypeStruct((rows, mixer_out.shape[1]), F32),
        ),
        in_specs=[vm] * 7,
        out_specs=(vm,) * 5,
        scratch_shapes=[
            pltpu.VMEM((2, VAL_DIM + 16, lanes), BF16),
            pltpu.VMEM((n, VAL_DIM + 16, lanes), BF16),
            pltpu.VMEM((model, mixer_out.shape[1]), BF16),
            pltpu.VMEM((n, rows, mixer_out.shape[1]), BF16),
            pltpu.VMEM((tokens // BLOCK, width, lanes), F32),
            pltpu.VMEM((tokens // BLOCK, width, lanes), F32),
            pltpu.SemaphoreType.DMA((n,)),
            pltpu.SemaphoreType.DMA((n,)),
            pltpu.SemaphoreType.DMA((n,)),
            pltpu.SemaphoreType.DMA((n,)),
        ],
        compiler_params=pltpu.CompilerParams(
            collective_id=0, has_side_effects=True, vmem_limit_bytes=24 * 1024 * 1024
        ),
        cost_estimate=pl.CostEstimate(
            flops=2 * 10**9, bytes_accessed=4 * 10**6, transcendentals=10**5
        ),
    )(token_grad, out_weight, mixer_out, query, key, value, log_decay)


def placement(ids, slots, cap):
    tokens = ids.shape[0]
    lane = lax.broadcasted_iota(jnp.int32, (tokens, 128), 1)
    first = ids[:, 0:1] == lane
    second = ids[:, 1:2] == lane
    named = jnp.where(first, 1.0, 0.0) + jnp.where(second, 1.0, 0.0)
    row = lax.broadcasted_iota(jnp.int32, (tokens, tokens), 0)
    col = lax.broadcasted_iota(jnp.int32, (tokens, tokens), 1)
    before = mm(jnp.where(col < row, 1.0, 0.0).astype(BF16), named.astype(BF16))
    at = before + (lane * cap).astype(F32)
    slot = lax.broadcasted_iota(jnp.int32, (tokens, slots), 1).astype(F32)

    def hot(mine):
        place = jnp.sum(jnp.where(mine, at, 0.0), axis=1, keepdims=True)
        return jnp.where(place == slot, 1.0, 0.0)

    return hot(first), hot(second)


def loop(start, stop, f):
    def body(d, _):
        f(d)
        return 0

    lax.fori_loop(start, stop, body, 0)


def span(index, width):
    return pl.ds(pl.multiple_of(index * width, width), width)


def dispatch_kernel(n, x, cot, ids, weights, outx, outc, sx, sc, s1, r1, s2, r2):
    me = lax.axis_index("sp")
    place = lax.axis_index("tp")
    half = lax.rem(place, 2)
    sibling = place + 1 - 2 * half
    barrier = greet(n, "sp")
    pl.semaphore_signal(barrier, inc=1, device_id={"tp": sibling})
    tokens, model = x.shape
    width = model // 2
    cap = outx.shape[1]
    slots = n * cap
    columns = span(half, width)
    hot0, hot1 = placement(ids[...], slots, cap)
    sent = mm((hot0 + hot1).astype(BF16), x[:, columns], 0, 0)
    sx[...] = sent.reshape(n, cap, width).astype(BF16)
    mine = cot[:, columns].astype(F32)
    w = weights[...]
    scaled = mm(hot0.astype(BF16), (w[:, 0:1] * mine).astype(BF16), 0, 0)
    scaled = scaled + mm(hot1.astype(BF16), (w[:, 1:2] * mine).astype(BF16), 0, 0)
    sc[...] = scaled.reshape(n, cap, width).astype(BF16)
    outx[me, :, columns] = sx[me]
    outc[me, :, columns] = sc[me]
    pl.semaphore_wait(barrier, n)
    pairs = ((0, sx, outx), (1, sc, outc))

    def first(i, source, out, d, slot):
        p = lax.rem(me + d, n)
        return pltpu.make_async_remote_copy(
            src_ref=source.at[p],
            dst_ref=out.at[slot, :, columns],
            send_sem=s1.at[i, d],
            recv_sem=r1.at[i, slot],
            device_id={"sp": p},
        )

    def second(i, src, out, slot, cols):
        return pltpu.make_async_remote_copy(
            src_ref=src,
            dst_ref=out.at[slot, :, cols],
            send_sem=s2.at[i, slot],
            recv_sem=r2.at[i, slot],
            device_id={"tp": sibling},
        )

    for i, source, out in pairs:
        loop(1, n, lambda d: first(i, source, out, d, me).start())
    for i, source, out in pairs:
        second(i, source.at[me], out, me, columns).start()
    for i, source, out in pairs:

        def forward(d):
            slot = lax.rem(me - d + n, n)
            first(i, source, out, d, slot).wait_recv()
            second(i, out.at[slot, :, columns], out, slot, columns).start()

        loop(1, n, forward)
    theirs = span(1 - half, width)
    for i, source, out in pairs:
        loop(0, n, lambda s: second(i, source.at[s], out, s, theirs).wait_recv())
        loop(1, n, lambda d: first(i, source, out, d, me).wait_send())
        loop(0, n, lambda s: second(i, source.at[s], out, s, columns).wait_send())


def dispatch(x, cot, ids, weights):
    n = lax.axis_size("sp")
    tokens, model = x.shape
    cap = 2 * tokens // n
    vm = pl.BlockSpec(memory_space=pltpu.VMEM)
    shape = jax.ShapeDtypeStruct((n, cap, model), BF16)
    buffer = pltpu.VMEM((n, cap, model // 2), BF16)
    sems = pltpu.SemaphoreType.DMA((2, n))
    outs = pl.pallas_call(
        functools.partial(dispatch_kernel, n),
        out_shape=(shape, shape),
        in_specs=[vm] * 4,
        out_specs=(vm, vm),
        scratch_shapes=[buffer, buffer, sems, sems, sems, sems],
        compiler_params=pltpu.CompilerParams(
            collective_id=1, has_side_effects=True, vmem_limit_bytes=32 * 1024 * 1024
        ),
    )(x, cot, ids, weights)
    return [out.reshape(n * cap, model) for out in outs]


def return_kernel(
    n, part, cot, ids, tg, got, to_far, far, to_home, home, quarter,
    s1, r1, s2, r2, s3, r3, s4, r4,
):
    me = lax.axis_index("sp")
    place = lax.axis_index("tp")
    core = lax.rem(place, 2)
    side = lax.div(place, 2)
    sibling = place + 1 - 2 * core
    opposite = lax.rem(place + 2, 4)
    barrier = greet(n, "sp")
    pl.semaphore_signal(barrier, inc=1, device_id={"tp": sibling})
    pl.semaphore_signal(barrier, inc=1, device_id={"tp": opposite})
    tokens, model = cot.shape
    cap = part.shape[1]
    slots = n * cap
    wide, slim = model // 2, model // 4
    mine = span(2 * core + side, slim)
    other = span(2 * core + 1 - side, slim)
    pl.semaphore_wait(barrier, n + 1)

    def near(p):
        return pltpu.make_async_remote_copy(
            src_ref=part.at[p, :, span(1 - core, wide)],
            dst_ref=got.at[p],
            send_sem=s1.at[p],
            recv_sem=r1.at[p],
            device_id={"tp": sibling},
        )

    def across(p):
        return pltpu.make_async_remote_copy(
            src_ref=to_far.at[p],
            dst_ref=far.at[p],
            send_sem=s2.at[p],
            recv_sem=r2.at[p],
            device_id={"tp": opposite},
        )

    def back(d, slot):
        p = lax.rem(me + d, n)
        return pltpu.make_async_remote_copy(
            src_ref=to_home.at[p],
            dst_ref=home.at[slot],
            send_sem=s3.at[d],
            recv_sem=r3.at[slot],
            device_id={"sp": p},
        )

    def to(d):
        return lax.rem(me + d, n)

    loop(1, n + 1, lambda d: near(to(d)).start())
    hot0, hot1 = placement(ids[...], slots, cap)

    def stage_far(d):
        p = to(d)
        near(p).wait_recv()
        to_far[p] = (
            part[p, :, other].astype(F32) + got[p, :, span(1 - side, slim)].astype(F32)
        ).astype(BF16)

        @pl.when(d > 1)
        def _():
            across(to(d - 1)).start()

    loop(1, n + 1, stage_far)
    across(me).start()

    def stage_home(d):
        p = to(d)
        across(p).wait_recv()
        to_home[p] = (
            part[p, :, mine].astype(F32)
            + got[p, :, span(side, slim)].astype(F32)
            + far[p].astype(F32)
        ).astype(BF16)

        @pl.when(d > 1)
        def _():
            back(d - 1, me).start()

    loop(1, n + 1, stage_home)
    home[me] = to_home[me]
    loop(1, n, lambda d: back(d, to(d)).wait_recv())
    rows = home[...].astype(F32).reshape(slots, slim).astype(BF16)
    total = cot[:, mine].astype(F32) + mm(hot0.astype(BF16), rows)
    total = (total + mm(hot1.astype(BF16), rows)).astype(BF16)
    quarter[...] = total
    tg[:, mine] = total
    pieces = 4
    size = tokens // pieces

    def share(i, kind, src, cols, target):
        return pltpu.make_async_remote_copy(
            src_ref=src,
            dst_ref=tg.at[span(i, size), cols],
            send_sem=s4.at[kind, i],
            recv_sem=r4.at[kind, i],
            device_id={"tp": target},
        )

    def own(i):
        return quarter.at[span(i, size)]

    theirs = span(2 * (1 - core) + side, slim)
    theirs_far = span(2 * (1 - core) + 1 - side, slim)
    loop(0, pieces, lambda i: share(i, 0, own(i), mine, opposite).start())
    loop(0, pieces, lambda i: share(i, 1, own(i), mine, sibling).start())

    def relay(i):
        share(i, 0, own(i), other, opposite).wait_recv()
        share(i, 2, tg.at[span(i, size), other], other, sibling).start()

    loop(0, pieces, relay)
    loop(0, pieces, lambda i: share(i, 1, own(i), theirs, sibling).wait_recv())
    loop(0, pieces, lambda i: share(i, 2, own(i), theirs_far, sibling).wait_recv())
    loop(0, n, lambda p: near(p).wait_send())
    loop(0, n, lambda p: across(p).wait_send())
    loop(1, n, lambda d: back(d, me).wait_send())
    for kind, target in ((0, opposite), (1, sibling), (2, sibling)):
        loop(0, pieces, lambda i: share(i, kind, own(i), mine, target).wait_send())


def give_back(partial_value, cot, ids):
    n = lax.axis_size("sp")
    tokens, model = cot.shape
    cap = 2 * tokens // n
    vm = pl.BlockSpec(memory_space=pltpu.VMEM)
    slim = pltpu.VMEM((n, cap, model // 4), BF16)
    sems = pltpu.SemaphoreType.DMA((n,))
    shared = pltpu.SemaphoreType.DMA((3, 4))
    return pl.pallas_call(
        functools.partial(return_kernel, n),
        out_shape=jax.ShapeDtypeStruct((tokens, model), BF16),
        in_specs=[vm] * 3,
        out_specs=vm,
        scratch_shapes=[pltpu.VMEM((n, cap, model // 2), BF16), slim, slim, slim, slim]
        + [pltpu.VMEM((tokens, model // 4), BF16)]
        + [sems] * 6
        + [shared] * 2,
        compiler_params=pltpu.CompilerParams(
            collective_id=2, has_side_effects=True, vmem_limit_bytes=32 * 1024 * 1024
        ),
    )(partial_value.reshape(n, cap, model), cot, ids)


def shards(
    moe_input,
    cotangent,
    expert_ids,
    route_weights,
    gate_weight,
    up_weight,
    down_weight,
    out_weight,
    mixer_out,
    query_vectors,
    key_vectors,
    value_vectors,
    log_decay,
):
    routed, routed_cot = dispatch(moe_input, cotangent, expert_ids, route_weights)
    grad_gate, grad_up, grad_down, partial_value = expert_pass(
        routed, routed_cot, gate_weight[0], up_weight[0], down_weight[0]
    )
    token_grad = give_back(partial_value.astype(jnp.bfloat16), cotangent, expert_ids)
    gradients = attention_backward(
        token_grad, out_weight, mixer_out, query_vectors, key_vectors, value_vectors, log_decay
    )
    return (
        grad_gate[None],
        grad_up[None],
        grad_down[None],
        gradients[4],
        gradients[0],
        gradients[1],
        gradients[2],
        gradients[3],
    )


def solution(mesh):
    return jax.shard_map(
        shards,
        mesh=mesh,
        in_specs=(
            P("sp", None),
            P("sp", None),
            P("sp", None),
            P("sp", None),
            P("sp", None, "tp"),
            P("sp", None, "tp"),
            P("sp", "tp", None),
            P(None, "tp"),
            P("sp", "tp"),
            P("sp", "tp"),
            P("sp", "tp"),
            P("sp", "tp"),
            P("sp", "tp"),
        ),
        out_specs=(
            P("sp", None, "tp"),
            P("sp", None, "tp"),
            P("sp", "tp", None),
            P("sp", "tp"),
            P("sp", "tp"),
            P("sp", "tp"),
            P("sp", "tp"),
            P("sp", "tp"),
        ),
        check_vma=False,
    )
```

```python
import functools
import jax
import jax.numpy as jnp
from jax import lax
from jax.experimental import pallas as pl
from jax.experimental.pallas import tpu as pltpu
from jax.sharding import PartitionSpec as P

KEY_CHANNELS = 64
VAL_DIM = 128
BLOCK = 64
HIGHEST = lax.Precision.HIGHEST
F32 = jnp.float32
BF16 = jnp.bfloat16


def mm(a, b, ca=1, cb=0, precision=None):
    return lax.dot_general(
        a, b, (((ca,), (cb,)), ((), ())), precision=precision, preferred_element_type=F32
    )


def expert_pass(routed, routed_cot, gate_local, up_local, down_local):
    pre_gate = jnp.dot(routed, gate_local, preferred_element_type=jnp.float32)
    pre_up = jnp.dot(routed, up_local, preferred_element_type=jnp.float32)
    sigmoid_gate = jax.nn.sigmoid(pre_gate)
    activated = pre_gate * sigmoid_gate
    hidden = (activated * pre_up).astype(jnp.bfloat16)
    delta_hidden = jnp.dot(routed_cot, down_local.T, preferred_element_type=jnp.float32)
    grad_down = jnp.dot(hidden.T, routed_cot, preferred_element_type=jnp.float32).astype(
        jnp.bfloat16
    )
    delta_gate = (
        delta_hidden * pre_up * sigmoid_gate * (1.0 + pre_gate * (1.0 - sigmoid_gate))
    ).astype(jnp.bfloat16)
    delta_up = (delta_hidden * activated).astype(jnp.bfloat16)
    grad_gate = jnp.dot(routed.T, delta_gate, preferred_element_type=jnp.float32).astype(
        jnp.bfloat16
    )
    grad_up = jnp.dot(routed.T, delta_up, preferred_element_type=jnp.float32).astype(jnp.bfloat16)
    partial_value = jnp.dot(delta_gate, gate_local.T, preferred_element_type=jnp.float32)
    partial_value = partial_value + jnp.dot(
        delta_up, up_local.T, preferred_element_type=jnp.float32
    )
    return (grad_gate, grad_up, grad_down, partial_value)


def greet(n, axis):
    me = lax.axis_index(axis)
    barrier = pltpu.get_barrier_semaphore()

    def body(d, _):
        pl.semaphore_signal(barrier, inc=1, device_id={axis: lax.rem(me + d, n)})
        return 0

    lax.fori_loop(1, n, body, 0)
    return barrier


def attention_kernel(
    n, tg, ow, mo, q, k, v, a, gq, gk, gv, ga, gow,
    pay, recv, gsend, grecv, upd_s, upd_p, ssem, rsem, gssem, grsem,
):
    me = lax.axis_index("sp")
    barrier = greet(n, "sp")
    tokens, lanes = q.shape
    blocks = tokens // BLOCK
    width = v.shape[1]
    heads = width // VAL_DIM
    rows = gow.shape[0]
    scale = KEY_CHANNELS ** (-0.5)

    cot = mm(tg[...], ow[...]).astype(BF16)
    row = lax.broadcasted_iota(jnp.int32, (tokens, tokens), 0)
    col = lax.broadcasted_iota(jnp.int32, (tokens, tokens), 1)
    same = (row // BLOCK) == (col // BLOCK)
    causal = same & (col <= row)
    cum = mm(jnp.where(causal, 1.0, 0.0), a[...], precision=HIGHEST)

    def spread(at):
        return jnp.concatenate(
            [
                jnp.broadcast_to(cum[b * BLOCK + at : b * BLOCK + at + 1], (BLOCK, lanes))
                for b in range(blocks)
            ],
            axis=0,
        )

    mid = spread(BLOCK // 2 - 1)
    end = spread(BLOCK - 1)
    qf = q[...].astype(F32) * scale
    kf = k[...].astype(F32)
    up_mid = jnp.exp(cum - mid)
    down_mid = jnp.exp(mid - cum)
    from_start = jnp.exp(cum)
    to_end = jnp.exp(end - cum)
    q_mid = (qf * up_mid).astype(BF16)
    k_mid = (kf * down_mid).astype(BF16)
    q_start = (qf * from_start).astype(BF16)
    k_end = (kf * to_end).astype(BF16)
    total = [cum[(b + 1) * BLOCK - 1 : (b + 1) * BLOCK] for b in range(blocks)]
    keep = [jnp.exp(t) for t in total]
    hrow = lax.broadcasted_iota(jnp.int32, (width, lanes), 0) // VAL_DIM
    hcol = lax.broadcasted_iota(jnp.int32, (width, lanes), 1) // KEY_CHANNELS
    headed = hrow == hcol

    def part(x, b):
        return x[b * BLOCK : (b + 1) * BLOCK]

    values = v[...]
    for b in range(blocks):
        upd_s[b] = jnp.where(headed, mm(part(values, b), part(k_end, b), 0, 0), 0.0)
        upd_p[b] = jnp.where(headed, mm(part(cot, b), part(q_start, b), 0, 0), 0.0)
    state = jnp.zeros((width, lanes), F32)
    pull = jnp.zeros((width, lanes), F32)
    for b in range(blocks):
        state = keep[b] * state + upd_s[b]
    for b in reversed(range(blocks)):
        pull = keep[b] * pull + upd_p[b]
    kept = jnp.exp(functools.reduce(lambda x, y: x + y, total))
    kept_hi = kept.astype(BF16)
    kept_lo = (kept - kept_hi.astype(F32)).astype(BF16)
    tail = jnp.concatenate(
        [jnp.broadcast_to(kept_hi.astype(F32), (8, lanes)), jnp.broadcast_to(kept_lo.astype(F32), (8, lanes))],
        axis=0,
    ).astype(BF16)

    def compact(x):
        return functools.reduce(
            lambda s, t: s + t, [x[h * VAL_DIM : (h + 1) * VAL_DIM] for h in range(heads)]
        )

    def expand(x):
        return jnp.where(headed, jnp.concatenate([x] * heads, axis=0), 0.0)

    pay[0, :VAL_DIM, :] = compact(state).astype(BF16)
    pay[1, :VAL_DIM, :] = compact(pull).astype(BF16)
    pay[0, VAL_DIM:, :] = tail
    pay[1, VAL_DIM:, :] = tail
    for j in range(tg.shape[1] // 256):
        gsend[j * 256 : (j + 1) * 256, :] = mm(
            tg[:, j * 256 : (j + 1) * 256], mo[...], 0, 0
        ).astype(BF16)
    pl.semaphore_wait(barrier, n - 1)

    def state_copy(d, slot):
        p = lax.rem(me + d, n)
        return pltpu.make_async_remote_copy(
            src_ref=pay.at[jnp.where(p > me, 0, 1)],
            dst_ref=recv.at[slot],
            send_sem=ssem.at[d],
            recv_sem=rsem.at[slot],
            device_id={"sp": p},
        )

    def grad_copy(d, slot):
        p = lax.rem(me + d, n)
        return pltpu.make_async_remote_copy(
            src_ref=gsend.at[pl.ds(pl.multiple_of(p * rows, rows), rows)],
            dst_ref=grecv.at[slot],
            send_sem=gssem.at[d],
            recv_sem=grsem.at[slot],
            device_id={"sp": p},
        )

    def each(f):
        def body(d, _):
            f(d)
            return 0

        lax.fori_loop(1, n, body, 0)

    each(lambda d: state_copy(d, me).start())
    each(lambda d: grad_copy(d, me).start())

    head_lane = lax.broadcasted_iota(jnp.int32, (tokens, lanes), 1) // KEY_CHANNELS
    dq = jnp.zeros((tokens, lanes), F32)
    dk = jnp.zeros((tokens, lanes), F32)
    dv = []
    for h in range(heads):
        cot_h = cot[:, h * VAL_DIM : (h + 1) * VAL_DIM]
        val_h = values[:, h * VAL_DIM : (h + 1) * VAL_DIM]
        q_h = jnp.where(head_lane == h, qf * up_mid, 0.0).astype(BF16)
        scores = jnp.where(causal, mm(q_h, k_mid, 1, 1), 0.0).astype(BF16)
        dscores = jnp.where(causal, mm(cot_h, val_h, 1, 1), 0.0).astype(BF16)
        dq = jnp.where(head_lane == h, mm(dscores, k_mid), dq)
        dk = jnp.where(head_lane == h, mm(dscores, q_mid, 0, 0), dk)
        dv.append(mm(scores, cot_h, 0, 0))
    dq = dq * up_mid
    dk = dk * down_mid
    dv = jnp.concatenate(dv, axis=1)

    each(lambda d: state_copy(d, lax.rem(me + d, n)).wait_recv())

    def follow(p, carry):
        ends = recv[p, VAL_DIM:, :].astype(F32)
        return (ends[0:1] + ends[8:9]) * carry + recv[p, :VAL_DIM, :].astype(F32)

    zero = jnp.zeros((VAL_DIM, lanes), F32)
    state = expand(lax.fori_loop(0, me, follow, zero))
    pull = expand(lax.fori_loop(0, n - 1 - me, lambda i, c: follow(n - 1 - i, c), zero))
    dq_in, after = [], []
    for b in range(blocks):
        dq_in.append(mm(part(cot, b), state.astype(BF16)))
        state = keep[b] * state + upd_s[b]
        after.append(state)
    dk_in, dv_in, edge = [None] * blocks, [None] * blocks, [None] * blocks
    for b in reversed(range(blocks)):
        low = pull.astype(BF16)
        dk_in[b] = mm(part(values, b), low)
        dv_in[b] = mm(part(k_end, b), low, 1, 1)
        edge[b] = jnp.broadcast_to(
            jnp.sum(after[b] * pull, axis=0, keepdims=True), (BLOCK, lanes)
        )
        pull = keep[b] * pull + upd_p[b]
    dq = dq + jnp.concatenate(dq_in, axis=0) * from_start
    dk = dk + jnp.concatenate(dk_in, axis=0) * to_end
    dv = dv + jnp.concatenate(dv_in, axis=0)
    gq[...] = (dq * scale).astype(BF16)
    gk[...] = dk.astype(BF16)
    gv[...] = dv.astype(BF16)
    flux = qf * dq - kf * dk
    later = jnp.where(same & (col >= row), 1.0, 0.0)
    ga[...] = mm(later, flux, precision=HIGHEST) + jnp.concatenate(edge, axis=0)

    each(lambda d: grad_copy(d, lax.rem(me + d, n)).wait_recv())
    own = gsend[pl.ds(pl.multiple_of(me * rows, rows), rows), :].astype(F32)
    gow[...] = lax.fori_loop(
        1, n, lambda d, t: t + grecv[lax.rem(me + d, n)].astype(F32), own
    )
    each(lambda d: state_copy(d, me).wait_send())
    each(lambda d: grad_copy(d, me).wait_send())


def attention_backward(token_grad, out_weight, mixer_out, query, key, value, log_decay):
    n = lax.axis_size("sp")
    tokens, lanes = query.shape
    width = value.shape[1]
    model = token_grad.shape[1]
    rows = model // n
    vm = pl.BlockSpec(memory_space=pltpu.VMEM)
    return pl.pallas_call(
        functools.partial(attention_kernel, n),
        out_shape=(
            jax.ShapeDtypeStruct((tokens, lanes), BF16),
            jax.ShapeDtypeStruct((tokens, lanes), BF16),
            jax.ShapeDtypeStruct((tokens, width), BF16),
            jax.ShapeDtypeStruct((tokens, lanes), F32),
            jax.ShapeDtypeStruct((rows, mixer_out.shape[1]), F32),
        ),
        in_specs=[vm] * 7,
        out_specs=(vm,) * 5,
        scratch_shapes=[
            pltpu.VMEM((2, VAL_DIM + 16, lanes), BF16),
            pltpu.VMEM((n, VAL_DIM + 16, lanes), BF16),
            pltpu.VMEM((model, mixer_out.shape[1]), BF16),
            pltpu.VMEM((n, rows, mixer_out.shape[1]), BF16),
            pltpu.VMEM((tokens // BLOCK, width, lanes), F32),
            pltpu.VMEM((tokens // BLOCK, width, lanes), F32),
            pltpu.SemaphoreType.DMA((n,)),
            pltpu.SemaphoreType.DMA((n,)),
            pltpu.SemaphoreType.DMA((n,)),
            pltpu.SemaphoreType.DMA((n,)),
        ],
        compiler_params=pltpu.CompilerParams(
            collective_id=0, has_side_effects=True, vmem_limit_bytes=24 * 1024 * 1024
        ),
        cost_estimate=pl.CostEstimate(
            flops=2 * 10**9, bytes_accessed=4 * 10**6, transcendentals=10**5
        ),
    )(token_grad, out_weight, mixer_out, query, key, value, log_decay)


def placement(ids, slots, cap):
    tokens = ids.shape[0]
    lane = lax.broadcasted_iota(jnp.int32, (tokens, 128), 1)
    first = ids[:, 0:1] == lane
    second = ids[:, 1:2] == lane
    named = jnp.where(first, 1.0, 0.0) + jnp.where(second, 1.0, 0.0)
    row = lax.broadcasted_iota(jnp.int32, (tokens, tokens), 0)
    col = lax.broadcasted_iota(jnp.int32, (tokens, tokens), 1)
    before = mm(jnp.where(col < row, 1.0, 0.0).astype(BF16), named.astype(BF16))
    at = before + (lane * cap).astype(F32)
    slot = lax.broadcasted_iota(jnp.int32, (tokens, slots), 1).astype(F32)

    def hot(mine):
        place = jnp.sum(jnp.where(mine, at, 0.0), axis=1, keepdims=True)
        return jnp.where(place == slot, 1.0, 0.0)

    return hot(first), hot(second)


def loop(start, stop, f):
    def body(d, _):
        f(d)
        return 0

    lax.fori_loop(start, stop, body, 0)


def span(index, width):
    return pl.ds(pl.multiple_of(index * width, width), width)


def dispatch_kernel(n, x, cot, ids, weights, outx, outc, sx, sc, s1, r1, s2, r2):
    me = lax.axis_index("sp")
    place = lax.axis_index("tp")
    core = lax.rem(place, 2)
    side = lax.div(place, 2)
    sibling = place + 1 - 2 * core
    opposite = lax.rem(place + 2, 4)
    barrier = greet(n, "sp")
    pl.semaphore_signal(barrier, inc=1, device_id={"tp": sibling})
    pl.semaphore_signal(barrier, inc=1, device_id={"tp": opposite})
    tokens, model = x.shape
    width = model // 4
    cap = outx.shape[1]
    slots = n * cap
    columns = span(2 * core + side, width)
    other = span(2 * core + 1 - side, width)
    hot0, hot1 = placement(ids[...], slots, cap)
    sent = mm((hot0 + hot1).astype(BF16), x[:, columns], 0, 0)
    sx[...] = sent.reshape(n, cap, width).astype(BF16)
    mine = cot[:, columns].astype(F32)
    w = weights[...]
    scaled = mm(hot0.astype(BF16), (w[:, 0:1] * mine).astype(BF16), 0, 0)
    scaled = scaled + mm(hot1.astype(BF16), (w[:, 1:2] * mine).astype(BF16), 0, 0)
    sc[...] = scaled.reshape(n, cap, width).astype(BF16)
    outx[me, :, columns] = sx[me]
    outc[me, :, columns] = sc[me]
    pl.semaphore_wait(barrier, n + 1)
    pairs = ((0, sx, outx), (1, sc, outc))

    def first(i, source, out, d, slot):
        p = lax.rem(me + d, n)
        return pltpu.make_async_remote_copy(
            src_ref=source.at[p],
            dst_ref=out.at[slot, :, columns],
            send_sem=s1.at[i, d],
            recv_sem=r1.at[i, slot],
            device_id={"sp": p},
        )

    def second(i, kind, src, out, slot, cols):
        return pltpu.make_async_remote_copy(
            src_ref=src,
            dst_ref=out.at[slot, :, cols],
            send_sem=s2.at[2 * kind + i, slot],
            recv_sem=r2.at[2 * kind + i, slot],
            device_id={"tp": opposite if kind == 0 else sibling},
        )

    def relay(i, out, d):
        slot = lax.rem(me - d + n, n)
        second(i, 0, out.at[slot, :, other], out, slot, other).wait_recv()
        second(i, 2, out.at[slot, :, other], out, slot, other).start()

    for i, source, out in pairs:
        loop(1, n, lambda d: first(i, source, out, d, me).start())
    for i, source, out in pairs:
        for kind in (0, 1):
            second(i, kind, source.at[me], out, me, columns).start()
    for i, source, out in pairs:

        def forward(d):
            slot = lax.rem(me - d + n, n)
            first(i, source, out, d, slot).wait_recv()
            for kind in (0, 1):
                second(i, kind, out.at[slot, :, columns], out, slot, columns).start()
            relay(i, out, d - 1)

        loop(1, n, forward)
    for i, source, out in pairs:
        relay(i, out, n - 1)
    theirs = span(2 * (1 - core) + side, width)
    theirs_far = span(2 * (1 - core) + 1 - side, width)
    for i, source, out in pairs:
        loop(0, n, lambda s: second(i, 1, source.at[s], out, s, theirs).wait_recv())
        loop(0, n, lambda s: second(i, 2, source.at[s], out, s, theirs_far).wait_recv())
        loop(1, n, lambda d: first(i, source, out, d, me).wait_send())
        for kind in (0, 1, 2):
            loop(0, n, lambda s: second(i, kind, source.at[s], out, s, columns).wait_send())


def dispatch(x, cot, ids, weights):
    n = lax.axis_size("sp")
    tokens, model = x.shape
    cap = 2 * tokens // n
    vm = pl.BlockSpec(memory_space=pltpu.VMEM)
    shape = jax.ShapeDtypeStruct((n, cap, model), BF16)
    buffer = pltpu.VMEM((n, cap, model // 4), BF16)
    sems = pltpu.SemaphoreType.DMA((2, n))
    more = pltpu.SemaphoreType.DMA((6, n))
    outs = pl.pallas_call(
        functools.partial(dispatch_kernel, n),
        out_shape=(shape, shape),
        in_specs=[vm] * 4,
        out_specs=(vm, vm),
        scratch_shapes=[buffer, buffer, sems, sems, more, more],
        compiler_params=pltpu.CompilerParams(
            collective_id=1, has_side_effects=True, vmem_limit_bytes=32 * 1024 * 1024
        ),
    )(x, cot, ids, weights)
    return [out.reshape(n * cap, model) for out in outs]


def return_kernel(
    n, part, cot, ids, tg, got, to_far, far, to_home, home, quarter,
    s1, r1, s2, r2, s3, r3, s4, r4,
):
    me = lax.axis_index("sp")
    place = lax.axis_index("tp")
    core = lax.rem(place, 2)
    side = lax.div(place, 2)
    sibling = place + 1 - 2 * core
    opposite = lax.rem(place + 2, 4)
    barrier = greet(n, "sp")
    pl.semaphore_signal(barrier, inc=1, device_id={"tp": sibling})
    pl.semaphore_signal(barrier, inc=1, device_id={"tp": opposite})
    tokens, model = cot.shape
    cap = part.shape[1]
    slots = n * cap
    wide, slim = model // 2, model // 4
    mine = span(2 * core + side, slim)
    other = span(2 * core + 1 - side, slim)
    pl.semaphore_wait(barrier, n + 1)

    def near(p):
        return pltpu.make_async_remote_copy(
            src_ref=part.at[p, :, span(1 - core, wide)],
            dst_ref=got.at[p],
            send_sem=s1.at[p],
            recv_sem=r1.at[p],
            device_id={"tp": sibling},
        )

    def across(p):
        return pltpu.make_async_remote_copy(
            src_ref=to_far.at[p],
            dst_ref=far.at[p],
            send_sem=s2.at[p],
            recv_sem=r2.at[p],
            device_id={"tp": opposite},
        )

    def back(d, slot):
        p = lax.rem(me + d, n)
        return pltpu.make_async_remote_copy(
            src_ref=to_home.at[p],
            dst_ref=home.at[slot],
            send_sem=s3.at[d],
            recv_sem=r3.at[slot],
            device_id={"sp": p},
        )

    def to(d):
        return lax.rem(me + d, n)

    loop(1, n + 1, lambda d: near(to(d)).start())
    hot0, hot1 = placement(ids[...], slots, cap)

    def stage_far(d):
        p = to(d)
        near(p).wait_recv()
        to_far[p] = (
            part[p, :, other].astype(F32) + got[p, :, span(1 - side, slim)].astype(F32)
        ).astype(BF16)

        @pl.when(d > 1)
        def _():
            across(to(d - 1)).start()

    loop(1, n + 1, stage_far)
    across(me).start()

    def stage_home(d):
        p = to(d)
        across(p).wait_recv()
        to_home[p] = (
            part[p, :, mine].astype(F32)
            + got[p, :, span(side, slim)].astype(F32)
            + far[p].astype(F32)
        ).astype(BF16)

        @pl.when(d > 1)
        def _():
            back(d - 1, me).start()

    loop(1, n + 1, stage_home)
    home[me] = to_home[me]
    loop(1, n, lambda d: back(d, to(d)).wait_recv())
    rows = home[...].astype(F32).reshape(slots, slim).astype(BF16)
    total = cot[:, mine].astype(F32) + mm(hot0.astype(BF16), rows)
    total = (total + mm(hot1.astype(BF16), rows)).astype(BF16)
    quarter[...] = total
    tg[:, mine] = total
    pieces = 4
    size = tokens // pieces

    def share(i, kind, src, cols, target):
        return pltpu.make_async_remote_copy(
            src_ref=src,
            dst_ref=tg.at[span(i, size), cols],
            send_sem=s4.at[kind, i],
            recv_sem=r4.at[kind, i],
            device_id={"tp": target},
        )

    def own(i):
        return quarter.at[span(i, size)]

    theirs = span(2 * (1 - core) + side, slim)
    theirs_far = span(2 * (1 - core) + 1 - side, slim)
    loop(0, pieces, lambda i: share(i, 0, own(i), mine, opposite).start())
    loop(0, pieces, lambda i: share(i, 1, own(i), mine, sibling).start())

    def relay(i):
        share(i, 0, own(i), other, opposite).wait_recv()
        share(i, 2, tg.at[span(i, size), other], other, sibling).start()

    loop(0, pieces, relay)
    loop(0, pieces, lambda i: share(i, 1, own(i), theirs, sibling).wait_recv())
    loop(0, pieces, lambda i: share(i, 2, own(i), theirs_far, sibling).wait_recv())
    loop(0, n, lambda p: near(p).wait_send())
    loop(0, n, lambda p: across(p).wait_send())
    loop(1, n, lambda d: back(d, me).wait_send())
    for kind, target in ((0, opposite), (1, sibling), (2, sibling)):
        loop(0, pieces, lambda i: share(i, kind, own(i), mine, target).wait_send())


def give_back(partial_value, cot, ids):
    n = lax.axis_size("sp")
    tokens, model = cot.shape
    cap = 2 * tokens // n
    vm = pl.BlockSpec(memory_space=pltpu.VMEM)
    slim = pltpu.VMEM((n, cap, model // 4), BF16)
    sems = pltpu.SemaphoreType.DMA((n,))
    shared = pltpu.SemaphoreType.DMA((3, 4))
    return pl.pallas_call(
        functools.partial(return_kernel, n),
        out_shape=jax.ShapeDtypeStruct((tokens, model), BF16),
        in_specs=[vm] * 3,
        out_specs=vm,
        scratch_shapes=[pltpu.VMEM((n, cap, model // 2), BF16), slim, slim, slim, slim]
        + [pltpu.VMEM((tokens, model // 4), BF16)]
        + [sems] * 6
        + [shared] * 2,
        compiler_params=pltpu.CompilerParams(
            collective_id=2, has_side_effects=True, vmem_limit_bytes=32 * 1024 * 1024
        ),
    )(partial_value.reshape(n, cap, model), cot, ids)


def shards(
    moe_input,
    cotangent,
    expert_ids,
    route_weights,
    gate_weight,
    up_weight,
    down_weight,
    out_weight,
    mixer_out,
    query_vectors,
    key_vectors,
    value_vectors,
    log_decay,
):
    routed, routed_cot = dispatch(moe_input, cotangent, expert_ids, route_weights)
    grad_gate, grad_up, grad_down, partial_value = expert_pass(
        routed, routed_cot, gate_weight[0], up_weight[0], down_weight[0]
    )
    token_grad = give_back(partial_value.astype(jnp.bfloat16), cotangent, expert_ids)
    gradients = attention_backward(
        token_grad, out_weight, mixer_out, query_vectors, key_vectors, value_vectors, log_decay
    )
    return (
        grad_gate[None],
        grad_up[None],
        grad_down[None],
        gradients[4],
        gradients[0],
        gradients[1],
        gradients[2],
        gradients[3],
    )


def solution(mesh):
    return jax.shard_map(
        shards,
        mesh=mesh,
        in_specs=(
            P("sp", None),
            P("sp", None),
            P("sp", None),
            P("sp", None),
            P("sp", None, "tp"),
            P("sp", None, "tp"),
            P("sp", "tp", None),
            P(None, "tp"),
            P("sp", "tp"),
            P("sp", "tp"),
            P("sp", "tp"),
            P("sp", "tp"),
            P("sp", "tp"),
        ),
        out_specs=(
            P("sp", None, "tp"),
            P("sp", None, "tp"),
            P("sp", "tp", None),
            P("sp", "tp"),
            P("sp", "tp"),
            P("sp", "tp"),
            P("sp", "tp"),
            P("sp", "tp"),
        ),
        check_vma=False,
    )
```
